32 devices in a mesh: sp: 16 (over z, y, x), tp: 2 (over core).
Axes of the slice: x: 2, y: 2, z: 4, core: 2. Of those that a mesh axis runs over, the one named last changes fastest.
Arguments:
- residual: bfloat16 [2048, 2048], P(('sp', 'tp')), may hold values from -6 to 6
- query_wide: bfloat16 [2048, 1024], P('sp', 'tp'), may hold values from -6 to 6
- key_wide: bfloat16 [2048, 1024], P('sp', 'tp'), may hold values from -6 to 6
- value_wide: bfloat16 [2048, 2048], P('sp', 'tp'), may hold values from -6 to 6
- outgate_wide: bfloat16 [2048, 2048], P('sp', 'tp'), may hold values from -6 to 6
- gating_wide: float32 [3, 8, 2048], P(None, 'tp', 'sp'), may hold values from -4 to 240, as said below
- gain_wide: bfloat16 [2048], P('tp'), may hold values from 0.099609375 to 1.8984375
- readout_wide: bfloat16 [2048, 2048], P('tp'), may hold values from -0.109375 to 0.109375
- query_narrow: bfloat16 [2048, 512], P('sp', 'tp'), may hold values from -6 to 6
- key_narrow: bfloat16 [2048, 512], P('sp', 'tp'), may hold values from -6 to 6
- value_narrow: bfloat16 [2048, 1024], P('sp', 'tp'), may hold values from -6 to 6
- outgate_narrow: bfloat16 [2048, 1024], P('sp', 'tp'), may hold values from -6 to 6
- gating_narrow: float32 [3, 8, 2048], P(None, 'tp', 'sp'), may hold values from -4 to 240, as said below
- gain_narrow: bfloat16 [1024], P('tp'), may hold values from 0.099609375 to 1.8984375
- readout_narrow: bfloat16 [1024, 2048], P('tp'), may hold values from -0.109375 to 0.109375
- norm_gain: bfloat16 [2048], replicated, may hold values from 0.099609375 to 1.8984375
- gate_weight: bfloat16 [2048, 5632], P('sp', 'tp'), may hold values from -0.125 to 0.125
- up_weight: bfloat16 [2048, 5632], P('sp', 'tp'), may hold values from -0.125 to 0.125
- down_weight: bfloat16 [5632, 2048], P('tp', 'sp'), may hold values from -0.078125 to 0.078125
Outputs:
- mixed_out: bfloat16 [2048, 2048], P(('sp', 'tp'))
The draws below stay inside these ranges and needn't reach their ends.
Inputs may be any that keep to these rules, and one draw needn't show every extreme that they name: `gating_wide`: row 0 holds input gate pre-activations, row 1 forget gate pre-activations, row 2 an added log-decay that is zero or negative. `gating_narrow`: row 0 holds input gate pre-activations, row 1 forget gate pre-activations, row 2 an added log-decay that is zero or negative.
All inputs are finite; a program needn't handle non-finite values.
Results may differ from the reference program's by a relative error of at most 0.017.
Values may be sent and summed in bfloat16 or wider, within the bound.
No kernel may reach another device: no remote copies, remote signals or barrier semaphores. Data moves between devices by JAX's collectives and lax.ppermute only.
A program may use at most 128 MiB of HBM per device.

```python
import math
import jax
import jax.numpy as jnp
from jax import lax

D = 2048
FF = 5632
HEADS_A = 8
DK_A = 128
DV_A = 256
HEADS_B = 8
DK_B = 64
DV_B = 128
BLOCK = 64
TOK_DEV = 128
CONTEXT_LENGTH = 2048
N_TP = 2


def draw_gating(key, attention_tally):
    keys = jax.random.split(key, 10)
    incoming_matrix = jnp.clip(jax.random.normal(keys[0], (attention_tally, CONTEXT_LENGTH), jnp.float32), -4.0, 4.0)
    entry_ordinal = jnp.broadcast_to(jnp.arange(attention_tally)[:, None], (attention_tally, 4))
    threshold = 50
    fast = jax.random.randint(keys[5], (attention_tally,), 0, 100) < threshold
    base = jnp.where(fast, 4.0, math.log(CONTEXT_LENGTH) + 1.0)
    levels = jnp.repeat(jax.random.uniform(keys[6], (CONTEXT_LENGTH // TOK_DEV,), jnp.float32, -0.7, 0.7), TOK_DEV)
    jitter = jax.random.uniform(keys[7], (attention_tally, CONTEXT_LENGTH), jnp.float32, -1.0, 1.0)
    retention_factor = base[:, None] + levels[None, :] + jitter
    word_locations = jax.random.randint(keys[8], (attention_tally, 3), 0, CONTEXT_LENGTH)
    objective_scores = jnp.log(jax.random.uniform(keys[9], (attention_tally, 3), jnp.float32, 0.5, 0.8))
    admission_exponent = jnp.zeros((attention_tally, CONTEXT_LENGTH), jnp.float32).at[entry_ordinal[:, :3], word_locations].add(objective_scores)
    admission_exponent = jnp.maximum(admission_exponent, -4.0)
    return jnp.stack([incoming_matrix, retention_factor, admission_exponent])


def draw_gating_wide(key, part):
    return draw_gating(jax.random.fold_in(key, 11), HEADS_A)


def draw_gating_narrow(key, part):
    return draw_gating(jax.random.fold_in(key, 12), HEADS_B)


def steps_of(own_key, extent, cuts, low, largest):
    level, own = 1.0, jax.random.fold_in(own_key, 6)
    for position, shards_of in cuts:
        draws = jnp.exp(jax.random.uniform(jax.random.fold_in(own, position), (shards_of,), jnp.float32, low / len(cuts), largest / len(cuts)))
        level = level * jnp.repeat(draws, extent[position] // shards_of).reshape([-1 if axis == position else 1 for axis in range(len(extent))])
    return level


def scatter_about(key, shape, width, bound, pieces=(), kind=jnp.bfloat16):
    array = jax.random.normal(key, shape, jnp.float32) * width
    if len(pieces) > 0:
        array = steps_of(key, shape, pieces, -0.22, 0.18) * array
    return jnp.clip(array, min=-bound, max=bound).astype(kind)


def setup_inputs(seed: int = 0) -> dict:
    splits = jax.random.split(jax.random.key(seed), 20)
    return {
        "residual": scatter_about(splits[0], (CONTEXT_LENGTH, D), 1.0, 6.0, ((0, 32),)),
        "query_wide": scatter_about(splits[1], (CONTEXT_LENGTH, HEADS_A * DK_A), 1.0, 6.0, ((0, 16), (1, 2))),
        "key_wide": scatter_about(splits[2], (CONTEXT_LENGTH, HEADS_A * DK_A), 1.0, 6.0, ((0, 16), (1, 2))),
        "value_wide": scatter_about(splits[3], (CONTEXT_LENGTH, HEADS_A * DV_A), 1.0, 6.0, ((0, 16), (1, 2))),
        "outgate_wide": scatter_about(splits[4], (CONTEXT_LENGTH, HEADS_A * DV_A), 1.0, 6.0, ((0, 16), (1, 2))),
        "gating_wide": draw_gating_wide(jax.random.fold_in(splits[19], 71), 0),
        "gain_wide": jnp.clip(1.0 + 0.18 * jax.random.normal(splits[6], (HEADS_A * DV_A,), jnp.float32), 0.099609375, 1.8984375).astype(jnp.bfloat16),
        "readout_wide": scatter_about(splits[7], (HEADS_A * DV_A, D), (HEADS_A * DV_A + HEADS_B * DV_B) ** -0.5, 0.109375, ((0, 2),)),
        "query_narrow": scatter_about(splits[8], (CONTEXT_LENGTH, HEADS_B * DK_B), 1.0, 6.0, ((0, 16), (1, 2))),
        "key_narrow": scatter_about(splits[9], (CONTEXT_LENGTH, HEADS_B * DK_B), 1.0, 6.0, ((0, 16), (1, 2))),
        "value_narrow": scatter_about(splits[10], (CONTEXT_LENGTH, HEADS_B * DV_B), 1.0, 6.0, ((0, 16), (1, 2))),
        "outgate_narrow": scatter_about(splits[11], (CONTEXT_LENGTH, HEADS_B * DV_B), 1.0, 6.0, ((0, 16), (1, 2))),
        "gating_narrow": draw_gating_narrow(jax.random.fold_in(splits[19], 71), 0),
        "gain_narrow": jnp.clip(1.0 + 0.18 * jax.random.normal(splits[13], (HEADS_B * DV_B,), jnp.float32), 0.099609375, 1.8984375).astype(jnp.bfloat16),
        "readout_narrow": scatter_about(splits[14], (HEADS_B * DV_B, D), (HEADS_A * DV_A + HEADS_B * DV_B) ** -0.5, 0.109375, ((0, 2),)),
        "norm_gain": jnp.clip(1.0 + 0.18 * jax.random.normal(splits[15], (D,), jnp.float32), 0.099609375, 1.8984375).astype(jnp.bfloat16),
        "gate_weight": scatter_about(splits[16], (D, FF), D ** -0.5, 0.125, ((0, 16), (1, 2))),
        "up_weight": scatter_about(splits[17], (D, FF), D ** -0.5, 0.125, ((0, 16), (1, 2))),
        "down_weight": scatter_about(splits[18], (FF, D), FF ** -0.5, 0.078125, ((0, 2), (1, 16))),
    }


def block_scan(query, key_rows, value, gating):
    tokens = query.shape[0]
    attention_tally = gating.shape[1]
    key_size = query.shape[1] // attention_tally
    value_size = value.shape[1] // attention_tally
    nblocks = tokens // BLOCK
    scale = key_size ** (-0.5)
    queries = query.astype(jnp.float32).reshape(nblocks, BLOCK, attention_tally, key_size)
    keys_all = key_rows.astype(jnp.float32).reshape(nblocks, BLOCK, attention_tally, key_size)
    values_all = value.astype(jnp.float32).reshape(nblocks, BLOCK, attention_tally, value_size)
    incoming_matrix = jnp.moveaxis(gating[0].reshape(attention_tally, nblocks, BLOCK), 1, 0)
    forget_log = jax.nn.log_sigmoid(gating[1]) + gating[2]
    forgets = jnp.moveaxis(forget_log.reshape(attention_tally, nblocks, BLOCK), 1, 0)
    causal = jnp.tril(jnp.ones((BLOCK, BLOCK), dtype=bool))

    def advance(carry, blocks):
        memory, level = carry
        q_block, k_block, v_block, in_block, f_block = blocks
        cumul = jnp.cumsum(f_block, axis=-1)
        logits = cumul[:, :, None] - cumul[:, None, :] + in_block[:, None, :]
        logits = jnp.where(causal, logits, -jnp.inf)
        carried = cumul + level[:, None]
        stab = jnp.maximum(carried, lax.optimization_barrier(jnp.max(logits, axis=-1)))
        weights = jnp.exp(logits - stab[:, :, None])
        scores = jnp.einsum('thd,shd->hts', q_block, k_block) * scale
        weighted = (scores * weights).astype(jnp.bfloat16).astype(jnp.float32)
        within = jnp.einsum('hts,shv->thv', weighted, v_block)
        earlier = jnp.einsum('thd,hdv->thv', q_block, memory, precision=lax.Precision.HIGHEST)
        earlier = earlier * jnp.exp(carried - stab).T[:, :, None]
        last = cumul[:, -1]
        tail = last[:, None] - cumul + in_block
        level_new = jnp.maximum(last + level, lax.optimization_barrier(jnp.max(tail, axis=-1)))
        tail_weights = jnp.exp(tail - level_new[:, None]) * scale
        scaled_keys = (k_block * tail_weights.T[:, :, None]).astype(jnp.bfloat16).astype(jnp.float32)
        memory_new = jnp.exp(last + level - level_new)[:, None, None] * memory
        memory_new = memory_new + jnp.einsum('shd,shv->hdv', scaled_keys, v_block)
        return ((memory_new, level_new), within + earlier)
    init = (jnp.zeros((attention_tally, key_size, value_size), jnp.float32), jnp.full((attention_tally,), -1e+30, jnp.float32))
    _, raw = lax.scan(advance, init, (queries, keys_all, values_all, incoming_matrix, forgets))
    return raw.reshape(tokens, attention_tally, value_size)

def finish(raw, gain, outgate):
    tokens, attention_tally, value_size = raw.shape
    normal_raw = raw * lax.rsqrt(lax.optimization_barrier(jnp.mean(raw * raw, axis=-1, keepdims=True)) + 1e-06)
    flat = normal_raw.reshape(tokens, attention_tally * value_size)
    flat = flat * gain.astype(jnp.float32) * jax.nn.sigmoid(outgate.astype(jnp.float32))
    return flat.astype(jnp.bfloat16)

def reference(residual, query_wide, key_wide, value_wide, outgate_wide, gating_wide, gain_wide, readout_wide, query_narrow, key_narrow, value_narrow, outgate_narrow, gating_narrow, gain_narrow, readout_narrow, norm_gain, gate_weight, up_weight, down_weight):
    gated_wide = finish(block_scan(query_wide, key_wide, value_wide, gating_wide), gain_wide, outgate_wide)
    gated_narrow = finish(block_scan(query_narrow, key_narrow, value_narrow, gating_narrow), gain_narrow, outgate_narrow)
    span_wide = gated_wide.shape[1] // N_TP
    span_narrow = gated_narrow.shape[1] // N_TP
    mixed = jnp.zeros(residual.shape, jnp.float32)
    for index in range(N_TP):
        part = jnp.dot(gated_wide[:, index * span_wide:(index + 1) * span_wide], readout_wide[index * span_wide:(index + 1) * span_wide], preferred_element_type=jnp.float32)
        part = part + jnp.dot(gated_narrow[:, index * span_narrow:(index + 1) * span_narrow], readout_narrow[index * span_narrow:(index + 1) * span_narrow], preferred_element_type=jnp.float32)
        mixed = mixed + part.astype(jnp.bfloat16).astype(jnp.float32)
    middle = (residual.astype(jnp.float32) + mixed).astype(jnp.bfloat16)
    middle_f = middle.astype(jnp.float32)
    normed = middle_f * lax.rsqrt(lax.optimization_barrier(jnp.mean(middle_f * middle_f, axis=-1, keepdims=True)) + 1e-06)
    normed = (normed * norm_gain.astype(jnp.float32)).astype(jnp.bfloat16)
    hidden_span = FF // N_TP
    back = jnp.zeros(residual.shape, jnp.float32)
    for index in range(N_TP):
        cols = slice(index * hidden_span, (index + 1) * hidden_span)
        gate = jnp.dot(normed, gate_weight[:, cols], preferred_element_type=jnp.float32)
        upper = jnp.dot(normed, up_weight[:, cols], preferred_element_type=jnp.float32)
        hidden = (jax.nn.silu(gate) * upper).astype(jnp.bfloat16)
        part = jnp.dot(hidden, down_weight[cols], preferred_element_type=jnp.float32)
        back = back + part.astype(jnp.bfloat16).astype(jnp.float32)
    return (middle_f + back).astype(jnp.bfloat16)
```

```python
import functools

import jax
import jax.numpy as jnp
from jax import lax
from jax.experimental import pallas as pl
from jax.experimental.pallas import tpu as pltpu
from jax.sharding import PartitionSpec as P

DK_A = 128
DK_B = 64
LANES = 128
HEAD_ROWS = 8
EMPTY = -1e30


VMEM = pl.BlockSpec(memory_space=pltpu.VMEM)
SMEM = pl.BlockSpec(memory_space=pltpu.SMEM)
ANY = pl.BlockSpec(memory_space=pl.ANY)


def log_sigmoid(x):
    return jnp.minimum(x, 0.0) - jnp.log1p(jnp.exp(-jnp.abs(x)))


def gates(wide_ref, narrow_ref, stage):
    wide, tokens = wide_ref.shape[1:]
    heads = wide + narrow_ref.shape[1]
    if heads < HEAD_ROWS:
        stage[...] = jnp.zeros_like(stage)
    for row in range(3):
        stage[row, :wide, :] = wide_ref[row]
        stage[row, wide:heads, :] = narrow_ref[row]
    forget = log_sigmoid(stage[1]) + stage[2]
    source = lax.broadcasted_iota(jnp.int32, (tokens, tokens), 0)
    target = lax.broadcasted_iota(jnp.int32, (tokens, tokens), 1)
    upper = jnp.where(source <= target, 1.0, 0.0)
    running = jnp.dot(
        forget, upper, precision=lax.Precision.HIGHEST, preferred_element_type=jnp.float32
    )
    return stage[0], running


def pieces_of(x):
    hi = x.astype(jnp.bfloat16).astype(jnp.float32)
    mid = (x - hi).astype(jnp.bfloat16).astype(jnp.float32)
    return hi, mid, x - hi - mid


def put_state(out_ref, memory, h, heads, at):
    dk, dv = memory.shape
    count = out_ref.shape[0]
    rows = heads * dk // count
    for j in range(dk // rows):
        for c in range(dv // LANES):
            part = memory[j * rows : (j + 1) * rows, c * LANES : (c + 1) * LANES]
            out_ref[h * (dk // rows) + j, at + c * rows : at + (c + 1) * rows, :] = part


def get_state(in_ref, h, heads, at, dk, dv):
    count = in_ref.shape[0]
    rows = heads * dk // count
    parts = []
    for j in range(dk // rows):
        block = h * (dk // rows) + j
        tiles = [in_ref[block, at + c * rows : at + (c + 1) * rows, :] for c in range(dv // LANES)]
        parts.append(jnp.concatenate(tiles, axis=1) if len(tiles) > 1 else tiles[0])
    return jnp.concatenate(parts, axis=0)


def state_kernel(sizes, spots, gw_ref, gn_ref, kw_ref, vw_ref, kn_ref, vn_ref, *refs):
    outs, stage = refs[:-1], refs[-1]
    heads_w, heads_n, dk_w, dv_w, dk_n, dv_n = sizes
    incoming, running = gates(gw_ref, gn_ref, stage)
    tokens = incoming.shape[1]
    total = running[:, tokens - 1 :]
    tail = total - running + incoming
    level = jnp.max(tail, axis=1, keepdims=True)
    row = lax.broadcasted_iota(jnp.int32, tail.shape, 0)
    scale = jnp.where(row < heads_w, dk_w**-0.5, dk_n**-0.5)
    weight = jnp.transpose(jnp.exp(tail - level) * scale)
    groups = (
        (kw_ref, vw_ref, 0, heads_w, dk_w, dv_w),
        (kn_ref, vn_ref, heads_w, heads_n, dk_n, dv_n),
    )
    for g, (k_ref, v_ref, base, heads, dk, dv) in enumerate(groups):
        for h in range(heads):
            keys = k_ref[:, h * dk : (h + 1) * dk].astype(jnp.float32)
            keys = (keys * weight[:, base + h : base + h + 1]).astype(jnp.bfloat16)
            memory = lax.dot_general(
                keys,
                v_ref[:, h * dv : (h + 1) * dv],
                (((0,), (0,)), ((), ())),
                preferred_element_type=jnp.float32,
            )
            memory = memory.astype(jnp.bfloat16)
            if spots:
                put_state(outs[0], memory, h, heads, spots[g])
            else:
                outs[g][h * dk : (h + 1) * dk, :] = memory
    column = lax.broadcasted_iota(jnp.int32, (HEAD_ROWS, LANES), 1)
    levels = []
    for value in (level, total):
        hi, mid, low = pieces_of(jnp.broadcast_to(value, (HEAD_ROWS, LANES)))
        part = jnp.where(column == 1, mid, jnp.where(column == 2, low, 0.0))
        part = jnp.where(column == 0, hi, part)
        levels.append(part.astype(jnp.bfloat16))
    levels = jnp.concatenate(levels, axis=0)
    if spots:
        for j in range(outs[0].shape[0]):
            outs[0][j, spots[2] : spots[2] + 2 * HEAD_ROWS, :] = levels
    else:
        outs[2][...] = levels


def prefix_kernel(heads_w, heads_n, spots, me_ref, got_ref, out_ref, in_ref):
    count = got_ref.shape[0]
    _, at_n, at_l = spots
    me = me_ref[0]
    head_w = me * heads_w // count
    head_n = heads_w + me * heads_n // count
    row = lax.broadcasted_iota(jnp.int32, (HEAD_ROWS, 1), 0)
    level = jnp.full((HEAD_ROWS, 1), EMPTY, jnp.float32)
    entry = level
    wide = jnp.zeros((at_n, LANES), jnp.float32)
    narrow = jnp.zeros((at_l - at_n, LANES), jnp.float32)

    def pick(value, head):
        return jnp.sum(jnp.where(row == head, value, 0.0), axis=0, keepdims=True)

    for d in range(count):
        entry = jnp.where(me == d, level, entry)
        out_ref[d, :at_n, :] = wide.astype(jnp.bfloat16)
        out_ref[d, at_n:at_l, :] = narrow.astype(jnp.bfloat16)
        if d == count - 1:
            break
        both = jnp.sum(got_ref[d, at_l:, :].astype(jnp.float32), axis=1, keepdims=True)
        theirs, total = both[:HEAD_ROWS], both[HEAD_ROWS:]
        after = jnp.maximum(level + total, theirs)
        old, new = jnp.exp(level + total - after), jnp.exp(theirs - after)
        wide = pick(old, head_w) * wide + pick(new, head_w) * got_ref[d, :at_n, :].astype(jnp.float32)
        theirs = got_ref[d, at_n:at_l, :].astype(jnp.float32)
        narrow = pick(old, head_n) * narrow + pick(new, head_n) * theirs
        level = after
    in_ref[...] = jnp.broadcast_to(entry, in_ref.shape)


def mixer_kernel(
    sizes,
    spots,
    gw_ref,
    gn_ref,
    in_ref,
    qw_ref,
    kw_ref,
    vw_ref,
    ow_ref,
    aw_ref,
    qn_ref,
    kn_ref,
    vn_ref,
    on_ref,
    an_ref,
    *refs,
):
    states, (rw_hbm, rn_hbm, out_ref, stage, rw_ref, rn_ref, sems) = refs[:-7], refs[-7:]
    heads_w, heads_n, dk_w, dv_w, dk_n, dv_n = sizes
    copies = (
        pltpu.make_async_copy(rw_hbm, rw_ref, sems.at[0]),
        pltpu.make_async_copy(rn_hbm, rn_ref, sems.at[1]),
    )
    for copy in copies:
        copy.start()
    incoming, running = gates(gw_ref, gn_ref, stage)
    tokens = incoming.shape[1]
    columns = jnp.transpose(running)
    t = lax.broadcasted_iota(jnp.int32, (tokens, tokens), 0)
    s = lax.broadcasted_iota(jnp.int32, (tokens, tokens), 1)
    causal = s <= t
    groups = (
        (qw_ref, kw_ref, vw_ref, ow_ref, aw_ref, 0, heads_w, dk_w, dv_w),
        (qn_ref, kn_ref, vn_ref, on_ref, an_ref, heads_w, heads_n, dk_n, dv_n),
    )
    gated = []
    for g, (q_ref, k_ref, v_ref, o_ref, a_ref, base, heads, dk, dv) in enumerate(groups):
        parts = []
        for h in range(heads):
            r = base + h
            q = q_ref[:, h * dk : (h + 1) * dk]
            k = k_ref[:, h * dk : (h + 1) * dk]
            v = v_ref[:, h * dv : (h + 1) * dv]
            here = columns[:, r : r + 1]
            logits = here - running[r : r + 1, :] + incoming[r : r + 1, :]
            logits = jnp.where(causal, logits, -jnp.inf)
            carried = here + in_ref[r : r + 1, 0:1]
            stab = jnp.maximum(carried, jnp.max(logits, axis=1, keepdims=True))
            weight = jnp.exp(logits - stab)
            scores = lax.dot_general(
                q, k, (((1,), (1,)), ((), ())), preferred_element_type=jnp.float32
            ) * (dk**-0.5)
            weighted = (scores * weight).astype(jnp.bfloat16)
            raw = jnp.dot(weighted, v, preferred_element_type=jnp.float32)
            if spots:
                state = get_state(states[0], h, heads, spots[g], dk, dv)
            else:
                state = states[g][h * dk : (h + 1) * dk, :]
            earlier = jnp.dot(q, state, preferred_element_type=jnp.float32)
            raw = raw + earlier * jnp.exp(carried - stab)
            raw = raw * lax.rsqrt(jnp.mean(raw * raw, axis=1, keepdims=True) + 1e-06)
            gain = a_ref[:, h * dv : (h + 1) * dv].astype(jnp.float32)
            gate = o_ref[:, h * dv : (h + 1) * dv].astype(jnp.float32)
            parts.append((raw * gain * jax.nn.sigmoid(gate)).astype(jnp.bfloat16))
        gated.append(jnp.concatenate(parts, axis=1) if heads > 1 else parts[0])
    for copy in copies:
        copy.wait()
    partial = jnp.dot(gated[0], rw_ref[...], preferred_element_type=jnp.float32)
    partial = partial + jnp.dot(gated[1], rn_ref[...], preferred_element_type=jnp.float32)
    out_ref[...] = partial.astype(jnp.bfloat16)


def gather_blocks(order_ref, pieces, weights, sems, axis):
    copies = []
    for piece in pieces:
        size = piece.shape[1 + axis]
        for m in range(piece.shape[0]):
            at = pl.ds(pl.multiple_of(order_ref[len(copies)] * size, size), size)
            target = weights.at[at, :] if axis == 0 else weights.at[:, at]
            copies.append(pltpu.make_async_copy(piece.at[m], target, sems.at[len(copies)]))
            copies[-1].start()
    return copies


def first_kernel(main, rest, order_ref, x_ref, *refs):
    pieces, (hidden_ref, weights, sems) = refs[:-3], refs[-3:]
    for copy in gather_blocks(order_ref, pieces, weights, sems, 0):
        copy.wait()
    both = jnp.dot(x_ref[...], weights[...], preferred_element_type=jnp.float32)
    if main:
        gate, upper = both[:, :main], both[:, main : 2 * main]
        hidden_ref[:, :main] = (jax.nn.silu(gate) * upper).astype(jnp.bfloat16)
    if rest:
        gate = both[:, 2 * main : 2 * main + rest]
        upper = both[:, 2 * main + rest :]
        hidden_ref[:, main:] = (jax.nn.silu(gate) * upper).astype(jnp.bfloat16)


def second_kernel(order_ref, hidden_ref, *refs):
    pieces, (out_ref, weights, sems) = refs[:-3], refs[-3:]
    for copy in gather_blocks(order_ref, pieces, weights, sems, 1):
        copy.wait()
    out = jnp.dot(hidden_ref[...], weights[...], preferred_element_type=jnp.float32)
    out_ref[...] = out.astype(jnp.bfloat16)


INNER = 4


def shift(x, k):
    count = lax.axis_size("sp")
    return lax.ppermute(x, "sp", [(j, (j + INNER * k) % count) for j in range(count)])


def flip(x, bits):
    return lax.ppermute(x, "sp", [(j, j ^ bits) for j in range(lax.axis_size("sp"))])


def across(x):
    return lax.ppermute(x, "tp", [(0, 1), (1, 0)])


def cost(flops, moved):
    return pl.CostEstimate(flops=int(flops), bytes_accessed=int(moved), transcendentals=0)


def cut(matrix, axis, place, main, rest, groups):
    parts = []
    if main:
        parts.append(lax.dynamic_slice_in_dim(matrix, place * main, main, axis))
    if rest:
        parts.append(lax.dynamic_slice_in_dim(matrix, groups * main + place * rest, rest, axis))
    return parts


def join(parts, axis):
    return jnp.concatenate(parts, axis=axis) if len(parts) > 1 else parts[0]


def round_up(n, m):
    return -(-n // m) * m


def exchange(x):
    return lax.all_to_all(x, "sp", 0, 0, tiled=True)


def mixer(
    query_wide, key_wide, value_wide, outgate_wide, gating_wide, gain_wide, readout_wide,
    query_narrow, key_narrow, value_narrow, outgate_narrow, gating_narrow, gain_narrow, readout_narrow,
):
    count = lax.axis_size("sp")
    tokens = query_wide.shape[0]
    width = readout_wide.shape[1]
    heads_w, heads_n = gating_wide.shape[1], gating_narrow.shape[1]
    dv_w, dv_n = value_wide.shape[1] // heads_w, value_narrow.shape[1] // heads_n
    sizes = (heads_w, heads_n, DK_A, dv_w, DK_B, dv_n)
    rows_w, rows_n = heads_w * DK_A // count, heads_n * DK_B // count
    lines_w, lines_n = rows_w * dv_w // LANES, rows_n * dv_n // LANES
    at_n = round_up(lines_w, 16)
    at_l = at_n + round_up(lines_n, 16)
    spots = (0, at_n, at_l)
    packed = rows_w % 16 == 0 and rows_n % 16 == 0
    inside = spots if packed else None
    stage = pltpu.VMEM((3, HEAD_ROWS, tokens), jnp.float32)
    total = (count, at_l + 2 * HEAD_ROWS, LANES)
    if packed:
        shapes = (total,)
    else:
        shapes = ((heads_w * DK_A, dv_w), (heads_n * DK_B, dv_n), (2 * HEAD_ROWS, LANES))
    outs = pl.pallas_call(
        functools.partial(state_kernel, sizes, inside),
        out_shape=[jax.ShapeDtypeStruct(shape, jnp.bfloat16) for shape in shapes],
        in_specs=[VMEM] * 6,
        out_specs=[VMEM] * len(shapes),
        scratch_shapes=[stage],
        cost_estimate=cost(3e8, 1e6),
        name="states",
    )(gating_wide, gating_narrow, key_wide, value_wide, key_narrow, value_narrow)
    if packed:
        payload = outs[0]
    else:
        wide = outs[0].reshape(count, lines_w, LANES)
        narrow = outs[1].reshape(count, lines_n, LANES)
        payload = jnp.concatenate(
            [
                jnp.pad(wide, ((0, 0), (0, at_n - lines_w), (0, 0))),
                jnp.pad(narrow, ((0, 0), (0, at_l - at_n - lines_n), (0, 0))),
                jnp.broadcast_to(outs[2], (count,) + outs[2].shape),
            ],
            axis=1,
        )
    got = exchange(payload)
    me = lax.axis_index("sp").reshape(1)
    before, entry = pl.pallas_call(
        functools.partial(prefix_kernel, heads_w, heads_n, spots),
        out_shape=[
            jax.ShapeDtypeStruct((count, at_l, LANES), jnp.bfloat16),
            jax.ShapeDtypeStruct((HEAD_ROWS, LANES), jnp.float32),
        ],
        in_specs=[SMEM, VMEM],
        out_specs=[VMEM] * 2,
        cost_estimate=cost(1e8, 1e6),
        name="prefix",
    )(me, got)
    before = exchange(before)
    if packed:
        states = (before,)
    else:
        states = (
            before[:, :lines_w].reshape(heads_w * DK_A, dv_w),
            before[:, at_n : at_n + lines_n].reshape(heads_n * DK_B, dv_n),
        )
    return pl.pallas_call(
        functools.partial(mixer_kernel, sizes, inside),
        out_shape=jax.ShapeDtypeStruct((tokens, width), jnp.bfloat16),
        in_specs=[VMEM] * (13 + len(states)) + [ANY] * 2,
        out_specs=VMEM,
        scratch_shapes=[
            stage,
            pltpu.VMEM(readout_wide.shape, jnp.bfloat16),
            pltpu.VMEM(readout_narrow.shape, jnp.bfloat16),
            pltpu.SemaphoreType.DMA((2,)),
        ],
        cost_estimate=cost(2e9, 8e6),
        name="mixer",
    )(
        gating_wide, gating_narrow, entry,
        query_wide, key_wide, value_wide, outgate_wide, gain_wide.reshape(1, -1),
        query_narrow, key_narrow, value_narrow, outgate_narrow, gain_narrow.reshape(1, -1),
        *states, readout_wide, readout_narrow,
    )


def spread(block, others):
    first, rest = block[None], jnp.stack(others) if others else None
    pieces = []
    for part in (first, rest):
        if part is not None:
            pieces.append(part)
            pieces.extend(flip(part, bits) for bits in range(1, INNER))
    return pieces


def body(
    residual,
    query_wide,
    key_wide,
    value_wide,
    outgate_wide,
    gating_wide,
    gain_wide,
    readout_wide,
    query_narrow,
    key_narrow,
    value_narrow,
    outgate_narrow,
    gating_narrow,
    gain_narrow,
    readout_narrow,
    norm_gain,
    gate_weight,
    up_weight,
    down_weight,
):
    count, cores = lax.axis_size("sp"), lax.axis_size("tp")
    groups = count // INNER
    here, core = lax.axis_index("sp"), lax.axis_index("tp")
    group, place = here // INNER, here % INNER
    units = gate_weight.shape[1] // groups
    main = units // LANES * LANES
    rest = units - main
    rows, width = residual.shape

    ups, downs = [], []
    for k in range(groups):
        to = (group + k) % groups
        gate = cut(gate_weight, 1, to, main, rest, groups)
        upper = cut(up_weight, 1, to, main, rest, groups)
        block = join([part for pair in zip(gate, upper) for part in pair], 1)
        ups.append(shift(block, k) if k else block)
    for k in range(groups):
        to = (group + k) % groups
        block = join(cut(down_weight, 0, to, main, rest, groups), 0)
        downs.append(shift(block, k) if k else block)
    up_pieces = spread(ups[0], ups[1:])
    down_pieces = spread(downs[0], downs[1:])
    order = []
    for ks in ((0,), tuple(range(1, groups))):
        for bits in range(INNER):
            order.extend((group - k) % groups * INNER + (place ^ bits) for k in ks)
    order = jnp.stack(order).astype(jnp.int32)

    mixed = mixer(
        query_wide, key_wide, value_wide, outgate_wide, gating_wide, gain_wide, readout_wide,
        query_narrow, key_narrow, value_narrow, outgate_narrow, gating_narrow, gain_narrow, readout_narrow,
    )
    if cores == 2:
        keep = lax.dynamic_slice_in_dim(mixed, core * rows, rows, 0)
        mixed = across(lax.dynamic_slice_in_dim(mixed, (1 - core) * rows, rows, 0))
        mixed = keep.astype(jnp.float32) + mixed.astype(jnp.float32)
    else:
        mixed = lax.psum_scatter(mixed, "tp", scatter_dimension=0, tiled=True)
    middle = (residual.astype(jnp.float32) + mixed.astype(jnp.float32)).astype(jnp.bfloat16)
    middle_f = middle.astype(jnp.float32)
    normed = middle_f * lax.rsqrt(jnp.mean(middle_f * middle_f, axis=-1, keepdims=True) + 1e-06)
    normed = (normed * norm_gain.astype(jnp.float32)).astype(jnp.bfloat16)

    mine = jnp.concatenate([shift(normed, k) if k else normed for k in range(groups)], axis=0)
    if cores == 2:
        x = jnp.concatenate([mine, across(mine)], axis=0)
    else:
        x = lax.all_gather(mine, "tp", axis=0, tiled=True)

    hidden = pl.pallas_call(
        functools.partial(first_kernel, main, rest),
        out_shape=jax.ShapeDtypeStruct((x.shape[0], units), jnp.bfloat16),
        in_specs=[SMEM, VMEM] + [ANY] * len(up_pieces),
        out_specs=VMEM,
        scratch_shapes=[
            pltpu.VMEM((width, 2 * units), jnp.bfloat16),
            pltpu.SemaphoreType.DMA((count,)),
        ],
        cost_estimate=cost(2 * x.shape[0] * width * 2 * units, 1e7),
        name="gate_up",
    )(order, x, *up_pieces)
    if down_weight.shape[1] % LANES == 0:
        y = pl.pallas_call(
            second_kernel,
            out_shape=jax.ShapeDtypeStruct(x.shape, jnp.bfloat16),
            in_specs=[SMEM, VMEM] + [ANY] * len(down_pieces),
            out_specs=VMEM,
            scratch_shapes=[
                pltpu.VMEM((units, width), jnp.bfloat16),
                pltpu.SemaphoreType.DMA((count,)),
            ],
            cost_estimate=cost(2 * x.shape[0] * width * units, 1e7),
            name="down",
        )(order, hidden, *down_pieces)
    else:
        stacked = jnp.concatenate(down_pieces, axis=0)[jnp.argsort(order)]
        stacked = jnp.moveaxis(stacked, 0, 1).reshape(units, width)
        y = jnp.dot(hidden, stacked, preferred_element_type=jnp.float32).astype(jnp.bfloat16)

    if cores == 2:
        half = x.shape[0] // 2
        y = y[:half].astype(jnp.float32) + across(y[half:]).astype(jnp.float32)
    else:
        y = lax.psum_scatter(y, "tp", scatter_dimension=0, tiled=True).astype(jnp.float32)
    out = middle_f + y[:rows]
    for k in range(1, groups):
        part = y[k * rows : (k + 1) * rows].astype(jnp.bfloat16)
        out = out + shift(part, -k).astype(jnp.float32)
    return out.astype(jnp.bfloat16)


def solution(mesh):
    in_specs = (
        P(("sp", "tp"), None),
        P("sp", "tp"),
        P("sp", "tp"),
        P("sp", "tp"),
        P("sp", "tp"),
        P(None, "tp", "sp"),
        P("tp"),
        P("tp", None),
        P("sp", "tp"),
        P("sp", "tp"),
        P("sp", "tp"),
        P("sp", "tp"),
        P(None, "tp", "sp"),
        P("tp"),
        P("tp", None),
        P(),
        P("sp", "tp"),
        P("sp", "tp"),
        P("tp", "sp"),
    )
    out_specs = P(("sp", "tp"), None)
    return jax.shard_map(body, mesh=mesh, in_specs=in_specs, out_specs=out_specs, check_vma=False)
```
